32 devices in a mesh: sp: 8 (over z, y), tp: 4 (over x, core).
Axes of the slice: x: 2, y: 2, z: 4, core: 2. Of those that a mesh axis runs over, the one named last changes fastest.
Arguments:
- residual: bfloat16 [8192, 2048], P(('sp', 'tp')), may hold values from -6 to 6
- first_group_queries: bfloat16 [8192, 1024], P('sp', 'tp'), may hold values from -6 to 6
- first_group_keys: bfloat16 [8192, 1024], P('sp', 'tp'), may hold values from -6 to 6
- second_group_queries: bfloat16 [8192, 512], P('sp', 'tp'), may hold values from -6 to 6
- second_group_keys: bfloat16 [8192, 512], P('sp', 'tp'), may hold values from -6 to 6
- primary_retain_switch_inputs: bfloat16 [8192, 1024], P('sp', 'tp'), may hold values from -12 to 16
- secondary_retain_switch_inputs: bfloat16 [8192, 512], P('sp', 'tp'), may hold values from -12 to 16
- timestep_fading_exponent: float32 [8192], P('sp'), may hold values from -2.1 to 0
- values: bfloat16 [2, 8192, 1024], P(None, 'sp', 'tp'), may hold values from -6 to 6
- output_gate_logits: bfloat16 [2, 8192, 1024], P(None, 'sp', 'tp'), may hold values from -6 to 6
- head_norm_gains: float32 [2, 1024], P(None, 'tp'), may hold values from 0.1 to 1.9
- output_projection: bfloat16 [2, 1024, 2048], P(None, 'tp'), may hold values from -0.125 to 0.125
- feedforward_norm_gain: float32 [2048], replicated, may hold values from 0.1 to 1.9
- gate_projection: bfloat16 [2048, 6144], P('sp', 'tp'), may hold values from -0.125 to 0.125
- up_projection: bfloat16 [2048, 6144], P('sp', 'tp'), may hold values from -0.125 to 0.125
- down_projection: bfloat16 [6144, 2048], P('tp', 'sp'), may hold values from -0.078125 to 0.078125
Outputs:
- layer_out: bfloat16 [8192, 2048], P(('sp', 'tp'))
The draws below stay inside these ranges and needn't reach their ends.
All inputs are finite; a program needn't handle non-finite values.
Results may differ from the reference program's by a relative error of at most 0.018.
Values may be sent and summed in bfloat16 or wider, within the bound.
No kernel may reach another device: no remote copies, remote signals or barrier semaphores. Data moves between devices by JAX's collectives and lax.ppermute only.
A program may use at most 128 MiB of HBM per device.

```python
import jax
import jax.numpy as jnp
from jax import lax

D = 2048
HEADS = 8
FIRST_KEY_SIZE = 128
SECOND_KEY_SIZE = 64
DV = 128
FF = 6144
BLOCK = 64
SEQ = 8192
N_TP = 4


def forget_draw(base_key, key_width):
    key_rank, key_factor, key_channel, key_jitter, key_long, key_level = jax.random.split(base_key, 6)
    ranking = jax.random.permutation(key_rank, HEADS)
    fast_count = HEADS // 2
    long_share = 0.5
    fast_mask = jnp.repeat((ranking < fast_count).astype(jnp.float32), key_width)
    slow_level = jnp.log(SEQ / 3.2)
    fast_level = -jnp.log(jnp.exp(16.0 / (0.6 * BLOCK)) - 1.0)
    long_mask = (jax.random.uniform(key_long, (HEADS * key_width,), jnp.float32) < long_share).astype(jnp.float32)
    spread_level = jax.random.uniform(key_level, (HEADS * key_width,), jnp.float32, jnp.log(4.0), slow_level)
    slow_channel = long_mask * slow_level + (1.0 - long_mask) * spread_level
    base_level = fast_mask * fast_level + (1.0 - fast_mask) * slow_channel
    factor = jax.random.uniform(key_factor, (SEQ // BLOCK, 1), jnp.float32, 0.0, jnp.log(4.0))
    factor = jnp.repeat(factor, BLOCK, axis=0)
    channel = jnp.clip(0.5 * jax.random.normal(key_channel, (1, HEADS * key_width), jnp.float32), -1.5, 1.5)
    jitter = jnp.clip(0.8 * jax.random.normal(key_jitter, (SEQ, HEADS * key_width), jnp.float32), -3.2, 3.2)
    result = base_level[None, :] - factor + channel + jitter
    return result.astype(jnp.bfloat16)


def draw_primary_retain_switch_inputs(key, part):
    return forget_draw(jax.random.fold_in(key, 11), FIRST_KEY_SIZE)


def draw_secondary_retain_switch_inputs(key, part):
    return forget_draw(jax.random.fold_in(key, 23), SECOND_KEY_SIZE)


def draw_timestep_fading_exponent(key, part):
    key_spot, key_loss = jax.random.split(jax.random.fold_in(key, 37))
    positions = jax.random.randint(key_spot, (3,), 0, SEQ)
    losses = jax.random.uniform(key_loss, (3,), jnp.float32, jnp.log(0.5), jnp.log(0.8))
    hits = jnp.arange(SEQ)[:, None] == positions[None, :]
    return jnp.sum(jnp.where(hits, losses[None, :], 0.0), axis=1).astype(jnp.float32)


def block_scale(stream_key, dims, shards, smallest, top_value):
    factor_of = 1.0
    for dim, shards_of in shards:
        draws = jax.random.uniform(jax.random.fold_in(jax.random.fold_in(stream_key, 6), dim), (shards_of,), jnp.float32, smallest / len(shards), top_value / len(shards))
        factor_of = factor_of * jnp.repeat(jnp.exp(draws), dims[dim] // shards_of).reshape((-1,) + (1,) * (len(dims) - 1 - dim))
    return factor_of


def scatter_about(key, shape, scale, limit, pieces=(), kind=jnp.bfloat16):
    entries = scale * jax.random.normal(key, shape, jnp.float32)
    if pieces:
        entries = entries * block_scale(key, shape, pieces, -0.22, 0.18)
    return jnp.clip(entries, -limit, limit).astype(kind)


def setup_inputs(seed: int = 0) -> dict:
    streams_of = jax.random.split(jax.random.key(seed), 17)
    return {
        "residual": scatter_about(streams_of[0], (SEQ, D), 1.0, 6.0, ((0, 32),)),
        "first_group_queries": scatter_about(streams_of[1], (SEQ, HEADS * FIRST_KEY_SIZE), 1.0, 6.0, ((0, 8), (1, 4))),
        "first_group_keys": scatter_about(streams_of[2], (SEQ, HEADS * FIRST_KEY_SIZE), 1.0, 6.0, ((0, 8), (1, 4))),
        "second_group_queries": scatter_about(streams_of[3], (SEQ, HEADS * SECOND_KEY_SIZE), 1.0, 6.0, ((0, 8), (1, 4))),
        "second_group_keys": scatter_about(streams_of[4], (SEQ, HEADS * SECOND_KEY_SIZE), 1.0, 6.0, ((0, 8), (1, 4))),
        "primary_retain_switch_inputs": draw_primary_retain_switch_inputs(jax.random.fold_in(streams_of[16], 71), 0),
        "secondary_retain_switch_inputs": draw_secondary_retain_switch_inputs(jax.random.fold_in(streams_of[16], 71), 0),
        "timestep_fading_exponent": draw_timestep_fading_exponent(jax.random.fold_in(streams_of[16], 71), 0),
        "values": scatter_about(streams_of[8], (2, SEQ, HEADS * DV), 1.0, 6.0, ((1, 8), (2, 4))),
        "output_gate_logits": scatter_about(streams_of[9], (2, SEQ, HEADS * DV), 1.0, 6.0, ((1, 8), (2, 4))),
        "head_norm_gains": jnp.clip(1.0 + 0.18 * jax.random.normal(streams_of[10], (2, HEADS * DV), jnp.float32), 0.1, 1.9),
        "output_projection": scatter_about(streams_of[11], (2, HEADS * DV, D), (2 * HEADS * DV) ** -0.5, 0.125, ((1, 4),)),
        "feedforward_norm_gain": jnp.clip(1.0 + 0.18 * jax.random.normal(streams_of[12], (D,), jnp.float32), 0.1, 1.9),
        "gate_projection": scatter_about(streams_of[13], (D, FF), D ** -0.5, 0.125, ((0, 8), (1, 4))),
        "up_projection": scatter_about(streams_of[14], (D, FF), D ** -0.5, 0.125, ((0, 8), (1, 4))),
        "down_projection": scatter_about(streams_of[15], (FF, D), FF ** -0.5, 0.078125, ((0, 4), (1, 8))),
    }


EPS = 1e-06
SOFTNESS_SCALE = 16.0
highest_precision = lax.Precision.HIGHEST

def blocks(source, block_count, head_count, key_width):
    return source.astype(jnp.float32).reshape(block_count, BLOCK, head_count, key_width).transpose(0, 2, 1, 3)

def mechanism(query_matrix_rows, key_matrix_rows, value_matrix_rows, decay_logarithm, key_width):
    block_count = query_matrix_rows.shape[0] // BLOCK
    query_blocks = blocks(query_matrix_rows, block_count, HEADS, key_width) * key_width ** (-0.5)
    key_blocks = blocks(key_matrix_rows, block_count, HEADS, key_width)
    value_blocks = blocks(value_matrix_rows, block_count, HEADS, DV)
    decay_blocks = jnp.cumsum(blocks(decay_logarithm, block_count, HEADS, key_width), axis=2)
    causal = jnp.tril(jnp.ones((BLOCK, BLOCK), dtype=bool))

    def advance(running_state, inputs):
        query_piece, key_piece, value_piece, decay_piece = inputs
        spread_log = decay_piece[:, :, None, :] - decay_piece[:, None, :, :]
        decay_grid = jnp.exp(jnp.where(causal[None, :, :, None], spread_log, -jnp.inf))
        scores = lax.optimization_barrier(jnp.sum(query_piece[:, :, None, :] * key_piece[:, None, :, :] * decay_grid, axis=-1))
        block_result = jnp.einsum('hij,hjv->hiv', scores, value_piece, precision=highest_precision)
        block_result = block_result + jnp.einsum('rus,rsp->rup', query_piece * jnp.exp(decay_piece), running_state, precision=highest_precision)
        final_log_decay = decay_piece[:, -1:, :]
        running_state = jnp.exp(final_log_decay[:, 0, :])[:, :, None] * running_state + jnp.einsum('qxe,qxt->qet', key_piece * jnp.exp(final_log_decay - decay_piece), value_piece, precision=highest_precision)
        return (running_state, block_result)
    zero_state = jnp.zeros((HEADS, key_width, DV), jnp.float32)
    _, outputs = lax.scan(advance, zero_state, (query_blocks, key_blocks, value_blocks, decay_blocks))
    return outputs.transpose(0, 2, 1, 3).reshape(query_matrix_rows.shape[0], HEADS, DV)

def gate_heads(head_out, gate_rows, gain_row):
    inverse = lax.rsqrt(lax.optimization_barrier(jnp.mean(head_out * head_out, axis=-1, keepdims=True)) + EPS)
    normed = (head_out * inverse).reshape(head_out.shape[0], -1) * gain_row
    return (jax.nn.silu(gate_rows.astype(jnp.float32)) * normed).astype(jnp.bfloat16)

def grouped_product(left_sides, right_sides):
    portion = left_sides[0].shape[1] // N_TP
    row_count = left_sides[0].shape[0]
    col_count = right_sides[0].shape[1]

    def add_group(group_index, summed):
        offset = (group_index * portion).astype(jnp.int32)
        partial_value = jnp.zeros((row_count, col_count), jnp.float32)
        for left_side, right_side in zip(left_sides, right_sides):
            partial_value = partial_value + jnp.dot(lax.dynamic_slice_in_dim(left_side, offset, portion, 1), lax.dynamic_slice_in_dim(right_side, offset, portion, 0), preferred_element_type=jnp.float32)
        rounded = lax.optimization_barrier(partial_value.astype(jnp.bfloat16))
        return summed + rounded.astype(jnp.float32)
    return lax.fori_loop(0, N_TP, add_group, jnp.zeros((row_count, col_count), jnp.float32))

def row_norm(source, gain_row):
    widened = source.astype(jnp.float32)
    inverse = lax.rsqrt(lax.optimization_barrier(jnp.mean(widened * widened, axis=-1, keepdims=True)) + EPS)
    return (widened * inverse * gain_row).astype(jnp.bfloat16)

def reference(residual, first_group_queries, first_group_keys, second_group_queries, second_group_keys, primary_retain_switch_inputs, secondary_retain_switch_inputs, timestep_fading_exponent, values, output_gate_logits, head_norm_gains, output_projection, feedforward_norm_gain, gate_projection, up_projection, down_projection):
    primary_fading_exponent = jax.nn.log_sigmoid(primary_retain_switch_inputs.astype(jnp.float32)) / SOFTNESS_SCALE + timestep_fading_exponent[:, None]
    secondary_fading_exponent = jax.nn.log_sigmoid(secondary_retain_switch_inputs.astype(jnp.float32)) / SOFTNESS_SCALE + timestep_fading_exponent[:, None]
    heads_a = mechanism(first_group_queries, first_group_keys, values[0], primary_fading_exponent, FIRST_KEY_SIZE)
    heads_b = mechanism(second_group_queries, second_group_keys, values[1], secondary_fading_exponent, SECOND_KEY_SIZE)
    gated_a = gate_heads(heads_a, output_gate_logits[0], head_norm_gains[0])
    gated_b = gate_heads(heads_b, output_gate_logits[1], head_norm_gains[1])
    attention = grouped_product((gated_a, gated_b), (output_projection[0], output_projection[1]))
    mid_rows = (residual.astype(jnp.float32) + attention).astype(jnp.bfloat16)
    normed = row_norm(mid_rows, feedforward_norm_gain)
    gate_sum = jnp.dot(normed, gate_projection, preferred_element_type=jnp.float32)
    up_sum = jnp.dot(normed, up_projection, preferred_element_type=jnp.float32)
    hidden = (jax.nn.silu(gate_sum) * up_sum).astype(jnp.bfloat16)
    down_sum = grouped_product((hidden,), (down_projection,))
    return (mid_rows.astype(jnp.float32) + down_sum).astype(jnp.bfloat16)
```

```python
import functools

import jax
import jax.numpy as jnp
from jax import lax
from jax.experimental import pallas as pl
from jax.experimental.pallas import tpu as pltpu
from jax.sharding import PartitionSpec as P

FIRST_KEY_SIZE = 128
SECOND_KEY_SIZE = 64
DV = 128
CHUNK = 128
PIECE = 32
PAD = 16
EPS = 1e-06
SOFTNESS_SCALE = 16.0
BF = jnp.bfloat16
F32 = jnp.float32
VMEM_LIMIT = 60 * 1024 * 1024


def nt(a, b):
    return lax.dot_general(a, b, (((1,), (1,)), ((), ())), preferred_element_type=F32)


def tn(a, b):
    return lax.dot_general(a, b, (((0,), (0,)), ((), ())), preferred_element_type=F32)


def nn(a, b):
    return lax.dot_general(a, b, (((1,), (0,)), ((), ())), preferred_element_type=F32)


def head_part(x, h, key, heads):
    if heads == 1:
        return x
    if key % 128 == 0:
        return x[:, h * key : (h + 1) * key]
    lanes = lax.broadcasted_iota(jnp.int32, (1, x.shape[1]), 1)
    return jnp.where((lanes >= h * key) & (lanes < (h + 1) * key), x, jnp.zeros_like(x))


def head_keys(x, h, key, heads):
    if heads == 1 or key % 128:
        return x
    return x[:, h * key : (h + 1) * key]


def state_kernel(
    ka, kb, va, vb, fa, fb, ts, cum_out, pack_out, acc, after, *, widths, keys
):
    step = pl.program_id(0)
    rows = ka.shape[0]

    @pl.when(step == 0)
    def _():
        acc[...] = jnp.zeros_like(acc)
        after[...] = jnp.zeros_like(after)

    ri = lax.broadcasted_iota(jnp.int32, (CHUNK, CHUNK), 0)
    ci = lax.broadcasted_iota(jnp.int32, (CHUNK, CHUNK), 1)
    tri = jnp.where(ri >= ci, 1.0, 0.0).astype(BF)
    base = 0
    for k, v, f, width, key in zip((ka, kb), (va, vb), (fa, fb), widths, keys):
        span = slice(base, base + width)
        heads = width // key
        suffix = after[0:1, span]
        total = None
        for c in reversed(range(rows // CHUNK)):
            rs = slice(c * CHUNK, (c + 1) * CHUNK)
            x = f[rs, :].astype(F32)
            g = (jnp.minimum(x, 0.0) - jnp.log1p(jnp.exp(-jnp.abs(x)))) * (
                1.0 / SOFTNESS_SCALE
            ) + ts[rs, :]
            hi = g.astype(BF)
            rest = g - hi.astype(F32)
            mid = rest.astype(BF)
            low = (rest - mid.astype(F32)).astype(BF)
            cum = nn(tri, hi) + nn(tri, mid) + nn(tri, low)
            cum_out[rs, span] = cum
            end = cum[CHUNK - 1 : CHUNK, :]
            kd = (k[rs, :].astype(F32) * jnp.exp(suffix + (end - cum))).astype(BF)
            suffix = suffix + end
            full = tn(v[0, rs, :], kd)
            part = None
            for h in range(heads):
                blk = full[h * DV : (h + 1) * DV, :]
                if heads > 1:
                    lanes = lax.broadcasted_iota(jnp.int32, (1, width), 1)
                    blk = jnp.where((lanes >= h * key) & (lanes < (h + 1) * key), blk, 0.0)
                part = blk if part is None else part + blk
            total = part if total is None else total + part
        acc[:, span] = acc[:, span] + total
        after[:, span] = jnp.broadcast_to(suffix, (after.shape[0], width))
        base += width

    @pl.when(step == pl.num_programs(0) - 1)
    def _():
        pack_out[0:DV, :] = acc[...]
        pack_out[DV : DV + PAD, :] = jnp.broadcast_to(
            jnp.exp(after[0:1, :]), (PAD, acc.shape[1])
        )


def state_pass(ka, kb, vals, fa, fb, ts, keys):
    rows = ka.shape[0]
    tile = min(rows, 256)
    n = rows // tile
    widths = (ka.shape[1], kb.shape[1])
    total = sum(widths)
    hv = vals.shape[2]
    back = lambda i: (n - 1 - i, 0)
    return pl.pallas_call(
        functools.partial(state_kernel, widths=widths, keys=keys),
        grid=(n,),
        in_specs=[
            pl.BlockSpec((tile, widths[0]), back),
            pl.BlockSpec((tile, widths[1]), back),
            pl.BlockSpec((1, tile, hv), lambda i: (0, n - 1 - i, 0)),
            pl.BlockSpec((1, tile, hv), lambda i: (1, n - 1 - i, 0)),
            pl.BlockSpec((tile, widths[0]), back),
            pl.BlockSpec((tile, widths[1]), back),
            pl.BlockSpec((tile, 1), back),
        ],
        out_specs=[
            pl.BlockSpec((tile, total), back),
            pl.BlockSpec((DV + PAD, total), lambda i: (0, 0)),
        ],
        out_shape=[
            jax.ShapeDtypeStruct((rows, total), F32),
            jax.ShapeDtypeStruct((DV + PAD, total), F32),
        ],
        scratch_shapes=[pltpu.VMEM((DV, total), F32), pltpu.VMEM((8, total), F32)],
        compiler_params=pltpu.CompilerParams(
            dimension_semantics=("arbitrary",), vmem_limit_bytes=VMEM_LIMIT
        ),
        name="state_pass",
    )(ka, kb, vals, vals, fa, fb, ts)


def local_kernel(
    qa, qb, ka, kb, va, vb, cum_ref, out, cross, state, before, *, widths, keys
):
    step = pl.program_id(0)
    rows = qa.shape[0]

    @pl.when(step == 0)
    def _():
        state[...] = jnp.zeros_like(state)
        before[...] = jnp.zeros_like(before)

    ri = lax.broadcasted_iota(jnp.int32, (CHUNK, CHUNK), 0)
    ci = lax.broadcasted_iota(jnp.int32, (CHUNK, CHUNK), 1)
    causal = ri >= ci
    pieces = CHUNK // PIECE
    for c in range(rows // CHUNK):
        rs = slice(c * CHUNK, (c + 1) * CHUNK)
        base = 0
        col = 0
        for q, k, v, width, key in zip((qa, qb), (ka, kb), (va, vb), widths, keys):
            span = slice(base, base + width)
            heads = width // key
            cum = cum_ref[rs, span]
            qf = q[rs, :].astype(F32) * key ** (-0.5)
            kf = k[rs, :].astype(F32)
            end = cum[CHUNK - 1 : CHUNK, :]
            q_in = qf * jnp.exp(cum)
            cross[rs, span] = (q_in * jnp.exp(before[0:1, span])).astype(BF)
            q_in = q_in.astype(BF)
            kd = (kf * jnp.exp(end - cum)).astype(BF)
            q_piece, k_piece = [], []
            for i in range(pieces):
                ref = cum[i * PIECE + PIECE // 2 : i * PIECE + PIECE // 2 + 1, :]
                top = (i + 1) * PIECE
                ps = slice(i * PIECE, top)
                q_piece.append((qf[ps] * jnp.exp(cum[ps] - ref)).astype(BF))
                k_piece.append((kf[:top] * jnp.exp(ref - cum[:top])).astype(BF))
            old = state[:, span]
            old_bf = old.astype(BF)
            full = tn(v[0, rs, :], kd)
            part = None
            for h in range(heads):
                strips = []
                for i in range(pieces):
                    s = nt(
                        head_part(q_piece[i], h, key, heads),
                        head_keys(k_piece[i], h, key, heads),
                    )
                    top = (i + 1) * PIECE
                    if top < CHUNK:
                        s = jnp.concatenate([s, jnp.zeros((PIECE, CHUNK - top), F32)], axis=1)
                    strips.append(s)
                scores = jnp.where(causal, jnp.concatenate(strips, axis=0), 0.0).astype(BF)
                vh = v[0, rs, h * DV : (h + 1) * DV]
                o = nn(scores, vh) + nt(
                    head_part(q_in, h, key, heads), head_keys(old_bf, h, key, heads)
                )
                out[rs, col + h * DV : col + (h + 1) * DV] = o
                blk = full[h * DV : (h + 1) * DV, :]
                if heads > 1:
                    lanes = lax.broadcasted_iota(jnp.int32, (1, width), 1)
                    blk = jnp.where((lanes >= h * key) & (lanes < (h + 1) * key), blk, 0.0)
                part = blk if part is None else part + blk
            state[:, span] = old * jnp.exp(end) + part
            before[:, span] = before[:, span] + end
            base += width
            col += heads * DV


def local_pass(qa, qb, ka, kb, vals, cum, keys):
    rows = ka.shape[0]
    tile = min(rows, 256)
    n = rows // tile
    widths = (ka.shape[1], kb.shape[1])
    total = sum(widths)
    hv = vals.shape[2]
    fwd = lambda i: (i, 0)
    return pl.pallas_call(
        functools.partial(local_kernel, widths=widths, keys=keys),
        grid=(n,),
        in_specs=[
            pl.BlockSpec((tile, widths[0]), fwd),
            pl.BlockSpec((tile, widths[1]), fwd),
            pl.BlockSpec((tile, widths[0]), fwd),
            pl.BlockSpec((tile, widths[1]), fwd),
            pl.BlockSpec((1, tile, hv), lambda i: (0, i, 0)),
            pl.BlockSpec((1, tile, hv), lambda i: (1, i, 0)),
            pl.BlockSpec((tile, total), fwd),
        ],
        out_specs=[
            pl.BlockSpec((tile, 2 * hv), fwd),
            pl.BlockSpec((tile, total), fwd),
        ],
        out_shape=[
            jax.ShapeDtypeStruct((rows, 2 * hv), F32),
            jax.ShapeDtypeStruct((rows, total), BF),
        ],
        scratch_shapes=[pltpu.VMEM((DV, total), F32), pltpu.VMEM((8, total), F32)],
        compiler_params=pltpu.CompilerParams(
            dimension_semantics=("arbitrary",), vmem_limit_bytes=VMEM_LIMIT
        ),
        name="local_pass",
    )(qa, qb, ka, kb, vals, vals, cum)


def finish_kernel(local, cross, state, gate_a, gate_b, gain, out, *, widths, keys):
    base = 0
    col = 0
    for g, (gate, width, key) in enumerate(zip((gate_a, gate_b), widths, keys)):
        span = slice(base, base + width)
        heads = width // key
        qx = cross[:, span]
        st = state[0:DV, span].astype(BF)
        for h in range(heads):
            cs = slice(col + h * DV, col + (h + 1) * DV)
            hs = slice(h * DV, (h + 1) * DV)
            o = local[:, cs] + nt(head_part(qx, h, key, heads), head_keys(st, h, key, heads))
            inv = lax.rsqrt(jnp.mean(o * o, axis=-1, keepdims=True) + EPS)
            z = gate[0, :, hs].astype(F32)
            out[:, cs] = (jax.nn.silu(z) * (o * inv * gain[g : g + 1, hs])).astype(BF)
        base += width
        col += heads * DV


def finish_pass(local, cross, state, gates, gains, widths, keys):
    rows = local.shape[0]
    tile = min(rows, 256)
    hv = gates.shape[2]
    total = sum(widths)
    fwd = lambda i: (i, 0)
    return pl.pallas_call(
        functools.partial(finish_kernel, widths=widths, keys=keys),
        grid=(rows // tile,),
        in_specs=[
            pl.BlockSpec((tile, 2 * hv), fwd),
            pl.BlockSpec((tile, total), fwd),
            pl.BlockSpec((DV + PAD, total), lambda i: (0, 0)),
            pl.BlockSpec((1, tile, hv), lambda i: (0, i, 0)),
            pl.BlockSpec((1, tile, hv), lambda i: (1, i, 0)),
            pl.BlockSpec((2, hv), lambda i: (0, 0)),
        ],
        out_specs=pl.BlockSpec((tile, 2 * hv), fwd),
        out_shape=jax.ShapeDtypeStruct((rows, 2 * hv), BF),
        compiler_params=pltpu.CompilerParams(
            dimension_semantics=("arbitrary",), vmem_limit_bytes=VMEM_LIMIT
        ),
        name="finish_pass",
    )(local, cross, state, gates, gates, gains)


def project_kernel(*refs, parts):
    gated = refs[:parts]
    weight = refs[parts : 2 * parts]
    residual, gain, mid, low, high, w, sem = refs[2 * parts :]
    copies = [pltpu.make_async_copy(weight[i], w.at[i], sem.at[i]) for i in range(parts)]
    for c in copies:
        c.start()
    acc = residual[...].astype(F32)
    hv = w.shape[2]
    for i in range(parts):
        copies[i].wait()
        acc = acc + nn(gated[i][:, :hv], w[i, 0]) + nn(gated[i][:, hv:], w[i, 1])
    m = acc.astype(BF)
    mid[...] = m
    m = m.astype(F32)
    inv = lax.rsqrt(jnp.mean(m * m, axis=-1, keepdims=True) + EPS)
    normed = (m * inv * gain[...]).astype(BF)
    half = low.shape[0]
    low[...] = normed[:half]
    high[...] = normed[half:]


def project(gated, weight, residual, gain):
    parts = len(gated)
    rows, width = residual.shape
    full = pl.BlockSpec(memory_space=pltpu.VMEM)
    return pl.pallas_call(
        functools.partial(project_kernel, parts=parts),
        in_specs=[full] * parts + [pl.BlockSpec(memory_space=pl.ANY)] * parts + [full, full],
        out_specs=[full, full, full],
        out_shape=[
            jax.ShapeDtypeStruct((rows, width), BF),
            jax.ShapeDtypeStruct((rows // 2, width), BF),
            jax.ShapeDtypeStruct((rows // 2, width), BF),
        ],
        scratch_shapes=[
            pltpu.VMEM((parts,) + weight[0].shape, BF),
            pltpu.SemaphoreType.DMA((parts,)),
        ],
        compiler_params=pltpu.CompilerParams(vmem_limit_bytes=VMEM_LIMIT),
        name="project",
    )(*gated, *weight, residual, gain)


def gate_up_kernel(*refs, groups, per, blocks):
    place = refs[0]
    xs = refs[1 : 1 + groups * per]
    gs = refs[1 + groups * per : 1 + groups * per + blocks]
    us = refs[1 + groups * per + blocks : 1 + groups * per + 2 * blocks]
    rest = refs[1 + groups * per + 2 * blocks :]
    outs = rest[:groups]
    x, wg, wu, xsem, wsem = rest[groups:]
    depth = gs[0].shape[0]
    piece = xs[0].shape[0]
    wcopies = []
    for i in range(blocks):
        off = pl.multiple_of(place[i] * depth, depth)
        wcopies.append(pltpu.make_async_copy(gs[i], wg.at[pl.ds(off, depth)], wsem.at[i]))
        wcopies.append(pltpu.make_async_copy(us[i], wu.at[pl.ds(off, depth)], wsem.at[blocks + i]))
    xcopies = [
        pltpu.make_async_copy(xs[i], x.at[pl.ds(i * piece, piece)], xsem.at[i])
        for i in range(groups * per)
    ]
    for c in wcopies + xcopies:
        c.start()
    for c in wcopies:
        c.wait()
    rows = per * piece
    for g in range(groups):
        for i in range(per):
            xcopies[g * per + i].wait()
        rs = slice(g * rows, (g + 1) * rows)
        a = nn(x[rs, :], wg[...])
        b = nn(x[rs, :], wu[...])
        outs[g][...] = (jax.nn.silu(a) * b).astype(BF)


def gate_up(xs, gs, us, place, groups):
    per = len(xs) // groups
    piece, width = xs[0].shape
    depth, hidden = gs[0].shape
    blocks = len(gs)
    anyspec = pl.BlockSpec(memory_space=pl.ANY)
    full = pl.BlockSpec(memory_space=pltpu.VMEM)
    return pl.pallas_call(
        functools.partial(gate_up_kernel, groups=groups, per=per, blocks=blocks),
        in_specs=[pl.BlockSpec(memory_space=pltpu.SMEM)]
        + [anyspec] * (len(xs) + 2 * blocks),
        out_specs=[full] * groups,
        out_shape=[jax.ShapeDtypeStruct((per * piece, hidden), BF)] * groups,
        scratch_shapes=[
            pltpu.VMEM((len(xs) * piece, width), BF),
            pltpu.VMEM((width, hidden), BF),
            pltpu.VMEM((width, hidden), BF),
            pltpu.SemaphoreType.DMA((len(xs),)),
            pltpu.SemaphoreType.DMA((2 * blocks,)),
        ],
        compiler_params=pltpu.CompilerParams(vmem_limit_bytes=VMEM_LIMIT),
        name="gate_up",
    )(place, *xs, *gs, *us)


def down_kernel(*refs, blocks):
    place, h = refs[:2]
    ws = refs[2 : 2 + blocks]
    keep, send, w, sem = refs[2 + blocks :]
    wide = ws[0].shape[1]
    copies = []
    for i in range(blocks):
        off = pl.multiple_of(place[i] * wide, wide)
        copies.append(pltpu.make_async_copy(ws[i], w.at[:, pl.ds(off, wide)], sem.at[i]))
    for c in copies:
        c.start()
    for c in copies:
        c.wait()
    rows = keep.shape[0]
    send[...] = nn(h[rows:, :], w[...]).astype(BF)
    keep[...] = nn(h[:rows, :], w[...]).astype(BF)


def down(h, ws, place):
    blocks = len(ws)
    rows, hidden = h.shape
    width = blocks * ws[0].shape[1]
    full = pl.BlockSpec(memory_space=pltpu.VMEM)
    return pl.pallas_call(
        functools.partial(down_kernel, blocks=blocks),
        in_specs=[pl.BlockSpec(memory_space=pltpu.SMEM), full]
        + [pl.BlockSpec(memory_space=pl.ANY)] * blocks,
        out_specs=[full, full],
        out_shape=[jax.ShapeDtypeStruct((rows // 2, width), BF)] * 2,
        scratch_shapes=[pltpu.VMEM((hidden, width), BF), pltpu.SemaphoreType.DMA((blocks,))],
        compiler_params=pltpu.CompilerParams(vmem_limit_bytes=VMEM_LIMIT),
        name="down",
    )(place, h, *ws)


def flip(x, axis, bits):
    n = lax.axis_size(axis)
    return lax.ppermute(x, axis, [(i, i ^ bits) for i in range(n)])


def add(a, b):
    return (a.astype(F32) + b.astype(F32)).astype(BF)


def entering(own, axis):
    place = lax.axis_index(axis)

    def join(earlier, later):
        rate = later[DV : DV + 1]
        return jnp.concatenate(
            [rate * earlier[:DV] + later[:DV], rate * earlier[DV:]], axis=0
        )

    total = own
    prefix = jnp.concatenate([jnp.zeros_like(own[:DV]), jnp.ones_like(own[DV:])], axis=0)
    bit = 1
    while bit < lax.axis_size(axis):
        other = flip(total.astype(BF), axis, bit).astype(F32)
        late = (place & bit) != 0
        prefix = jnp.where(late, join(other, prefix), prefix)
        first = jnp.where(late, other, total)
        second = jnp.where(late, total, other)
        total = join(first, second)
        bit *= 2
    return prefix


def gather_weight(own, other, split, bits):
    found = {0: own, split: flip(other, "sp", split)}
    for bit in bits:
        for r in list(found):
            found[r ^ bit] = flip(found[r], "sp", bit)
    return found


def per_device(
    residual,
    first_group_queries,
    first_group_keys,
    second_group_queries,
    second_group_keys,
    primary_retain_switch_inputs,
    secondary_retain_switch_inputs,
    timestep_fading_exponent,
    values,
    output_gate_logits,
    head_norm_gains,
    output_projection,
    feedforward_norm_gain,
    gate_projection,
    up_projection,
    down_projection,
):
    sp, tp = lax.axis_size("sp"), lax.axis_size("tp")
    s, t = lax.axis_index("sp"), lax.axis_index("tp")
    keys = (FIRST_KEY_SIZE, SECOND_KEY_SIZE)
    widths = (first_group_keys.shape[1], second_group_keys.shape[1])
    split = 2
    others = [4, 1] + [1 << i for i in range(3, sp.bit_length() - 1)]
    odd = (s & split) != 0

    def halves(w, axis):
        n = w.shape[axis] // 2
        lo = lax.slice_in_dim(w, 0, n, axis=axis)
        hi = lax.slice_in_dim(w, n, 2 * n, axis=axis)
        return jnp.where(odd, hi, lo), jnp.where(odd, lo, hi)

    gates = gather_weight(*halves(gate_projection, 1), split, others)
    ups = gather_weight(*halves(up_projection, 1), split, others)
    downs = gather_weight(*halves(down_projection, 0), split, others)
    order = sorted(gates)
    place = jnp.stack([s ^ r for r in order]).astype(jnp.int32)

    wide = {0: output_projection}
    bit = tp // 2
    while bit:
        for r in list(wide):
            wide[r ^ bit] = flip(wide[r], "tp", bit)
        bit //= 2

    cum, own = state_pass(
        first_group_keys,
        second_group_keys,
        values,
        primary_retain_switch_inputs,
        secondary_retain_switch_inputs,
        timestep_fading_exponent[:, None],
        keys,
    )
    local, cross = local_pass(
        first_group_queries,
        second_group_queries,
        first_group_keys,
        second_group_keys,
        values,
        cum,
        keys,
    )
    prefix = entering(own, "sp")
    gated = finish_pass(
        local, cross, prefix, output_gate_logits, head_norm_gains, widths, keys
    )
    rows = residual.shape[0]
    swapped = []
    for r in range(tp):
        piece = lax.dynamic_slice_in_dim(gated, (t ^ r) * rows, rows, 0)
        swapped.append(flip(piece, "tp", r) if r else piece)
    mid, low, high = project(
        swapped, [wide[r] for r in range(tp)], residual, feedforward_norm_gain[None, :]
    )

    tp_bits = [1 << i for i in range(1, tp.bit_length() - 1)]
    x_route = [("tp", b) for b in tp_bits]
    routes = (x_route + [("sp", split)], [("sp", split)] + x_route)

    def spread(x, route):
        found = {(0, 0): x}
        for axis, bit in route:
            for r, z in list(found):
                key = (r ^ bit, z) if axis == "tp" else (r, z ^ 1)
                found[key] = flip(found[(r, z)], axis, bit)
        for r, z in list(found):
            found[(r ^ 1, z)] = flip(found[(r, z)], "tp", 1)
        return found

    pieces = [spread(x, route) for x, route in zip((low, high), routes)]
    chips = [(r, z) for z in (1, 0) for r in reversed(range(0, tp, 2))]
    xs = [pieces[i][(r ^ c, z)] for r, z in chips for c in (0, 1) for i in (0, 1)]
    hidden = gate_up(
        xs, [gates[r] for r in order], [ups[r] for r in order], place, len(chips)
    )
    down_list = [downs[r] for r in order]
    down_place = place
    if down_list[0].shape[1] % 128:
        stack = jnp.stack(down_list)
        stack = stack[jnp.stack([s ^ r for r in range(sp)])]
        down_list = [jnp.swapaxes(stack, 0, 1).reshape(stack.shape[1], -1)]
        down_place = jnp.zeros((1,), jnp.int32)
    sums = {}
    for chip, h in zip(chips, hidden):
        keep, send = down(h, down_list, down_place)
        sums[chip] = add(keep, flip(send, "tp", 1))
    half = rows // 2
    final = []
    for i, route in enumerate(routes):
        part = {k: v[i * half : (i + 1) * half] for k, v in sums.items()}
        for axis, bit in route:
            for r, z in sorted(part, reverse=True):
                gone = (r & bit) if axis == "tp" else z
                if gone:
                    key = (r ^ bit, z) if axis == "tp" else (r, z ^ 1)
                    got = flip(part.pop((r, z)), axis, bit)
                    part[key] = add(part[key], got)
        final.append(part[(0, 0)])
    total = jnp.concatenate(final, axis=0).astype(F32)
    return (mid.astype(F32) + total).astype(BF)


def solution(mesh):
    return jax.shard_map(
        per_device,
        mesh=mesh,
        in_specs=(
            P(("sp", "tp"), None),
            P("sp", "tp"),
            P("sp", "tp"),
            P("sp", "tp"),
            P("sp", "tp"),
            P("sp", "tp"),
            P("sp", "tp"),
            P("sp"),
            P(None, "sp", "tp"),
            P(None, "sp", "tp"),
            P(None, "tp"),
            P(None, "tp", None),
            P(),
            P("sp", "tp"),
            P("sp", "tp"),
            P("tp", "sp"),
        ),
        out_specs=P(("sp", "tp"), None),
        check_vma=False,
    )
```
